256 devices in a mesh: sp: 64 (over z, y, core), tp: 4 (over x).
Axes of the slice: x: 4, y: 4, z: 8, core: 2. Of those that a mesh axis runs over, the one named last changes fastest.
Arguments:
- queries: bfloat16 [8192, 2048], P('sp', 'tp'), may hold values from -6 to 6
- keys: bfloat16 [8192, 512], P('sp', 'tp'), may hold values from -6 to 6
- values: bfloat16 [8192, 512], P('sp', 'tp'), may hold values from -6 to 6
- query_gain: float32 [128], replicated, may hold values from 0.3 to 7
- key_norm_gain: float32 [128], replicated, may hold values from 0.3 to 7
- out_weight: bfloat16 [2048, 2048], P('tp'), may hold values from -0.25 to 0.25
- residual: bfloat16 [8192, 2048], P(('sp', 'tp')), may hold values from -6 to 6
- norm_gain: float32 [2048], replicated, may hold values from 0.1 to 1.9
- expert_gate: bfloat16 [64, 2048, 3072], P('sp', None, 'tp'), may hold values from -0.125 to 0.125
- expert_up: bfloat16 [64, 2048, 3072], P('sp', None, 'tp'), may hold values from -0.125 to 0.125
- expert_down: bfloat16 [64, 3072, 2048], P('sp', 'tp'), may hold values from -0.109375 to 0.109375
- routes: int32 [8192, 2], P(('sp', 'tp')), may hold values from 0 to 63, all different within a row; in each aligned block of 32 rows (0 to 31, 32 to 63, ...) at most 2 rows name the same one
- route_weight: float32 [8192, 2], P(('sp', 'tp')), may hold values from 0.25 to 1
Outputs:
- mixed: bfloat16 [8192, 2048], P(('sp', 'tp'))
The draws below stay inside these ranges and needn't reach their ends.
Inputs may be any that keep to these rules, and one draw needn't show every extreme that they name: The two experts of a token differ. In each aligned block of 32 tokens (the tokens of one device), no expert is named by more than 2 routes, and in some block one expert is named by exactly 2.
All inputs are finite; a program needn't handle non-finite values.
Results may differ from the reference program's by a relative error of at most 0.013.
The reference program's roundings to bfloat16 on the way count: a program that leaves them out, or rounds other values in their place, can miss the bound.
Values may be sent and summed in bfloat16 or wider, within the bound.
A program may use at most 64 MiB of HBM per device.

```python
import math
import jax
import jax.numpy as jnp
import numpy as np
from jax import lax

D = 2048
QUERY_HEAD_COUNT = 16
KEY_VALUE_HEADS = 4
HEAD_SIZE = 128
FE = 3072
TOP = 2
GRID_W = 64
TOK_DEV = 128
SEQUENCE_TOKENS = 8192
EXPERTS = 64
CAP = 2
N_SP = 64
N_TP = 4


def shared_gain(key, salt_value):
    uniform_unit = jax.random.uniform(jax.random.fold_in(key, salt_value), (HEAD_SIZE,), jnp.float32)
    return jnp.exp(jnp.log(1.2) + uniform_unit * (jnp.log(2.5) - jnp.log(1.2)))


def draw_query_gain(key, part):
    return shared_gain(key, 102)


def draw_key_norm_gain(key, part):
    return shared_gain(key, 103)


def build_keys(key):
    base_sample = jnp.clip(jax.random.normal(jax.random.fold_in(key, 104), (SEQUENCE_TOKENS, KEY_VALUE_HEADS * HEAD_SIZE), jnp.float32), -6.0, 6.0)
    return base_sample


def draw_keys(key, part):
    return build_keys(key).astype(jnp.bfloat16)


def draw_queries(key, part):
    base_sample = jnp.clip(jax.random.normal(jax.random.fold_in(key, 105), (SEQUENCE_TOKENS, QUERY_HEAD_COUNT * HEAD_SIZE), jnp.float32), -6.0, 6.0)
    return base_sample.astype(jnp.bfloat16)


def levels(stream_key, dims, cuts, smallest, top_value):
    def one(position, shards_of):
        steps = jax.random.uniform(jax.random.fold_in(jax.random.fold_in(stream_key, 6), position), (shards_of,), jnp.float32, smallest / len(cuts), top_value / len(cuts))
        return jnp.repeat(jnp.exp(steps), dims[position] // shards_of).reshape((-1,) + (1,) * (len(dims) - position - 1))

    level = one(*cuts[0])
    for cut in cuts[1:]:
        level = level * one(*cut)
    return level


def assign_block(key, own, number, rows, amount, top, reach, skew):
    ranking = jax.random.permutation(key, amount)
    crowded, usual = portions_of(amount, rows * top, reach, skew, True), portions_of(amount, rows * top, reach, skew, False)
    places = jnp.arange(amount)

    def named(sizes, rotation):
        used = int((sizes > 0).sum())
        fixed = max(1, used // 4)
        shifted = fixed + (places - fixed + rotation * (used - fixed)) % max(1, amount - fixed)
        return jnp.zeros((amount,), jnp.int32).at[ranking[jnp.where(places < fixed, places, shifted)]].set(jnp.asarray(sizes, jnp.int32))

    sizes = jnp.where(number % 4 == 0, named(crowded, number // 4), named(usual, number - number // 4 - 1))
    mixed = jax.random.permutation(jax.random.fold_in(own, 3), amount)
    donor, sink = mixed[0:amount // 2 * 2:2], mixed[1:amount // 2 * 2:2]
    margin = jnp.minimum(sizes[donor] - 1, reach - sizes[sink]) // 2
    margin = jnp.where((donor == ranking[0]) | (sink == ranking[0]) | (sizes[sink] == 0), 0, jnp.maximum(margin, 0))
    shifted = jax.random.randint(jax.random.fold_in(own, 4), (amount // 2,), 0, 1 << 20) % (margin + 1)
    sizes = sizes.at[donor].add(-shifted).at[sink].add(shifted)
    labels = jnp.searchsorted(jnp.cumsum(sizes), jnp.arange(rows * top), side="right").astype(jnp.int32)
    grid = labels.reshape(top, rows).T
    grid = grid[jax.random.permutation(jax.random.fold_in(own, 1), rows)]
    rotation = jax.random.randint(jax.random.fold_in(own, 2), (rows, 1), 0, top)
    return jnp.take_along_axis(grid, (jnp.arange(top)[None, :] + rotation) % top, axis=1)


def portions_of(count, total, bound, skew, full):
    portions = [(1 << 20) // math.isqrt(standing ** skew) + 1 for standing in range(1, count + 1)]
    largest = bound if full else min(bound, max(-(-total // count), total * portions[0] // sum(portions)))
    least = 1 if total - largest >= count - 1 else 0
    holding, spare = [largest] + [least] * (count - 1), total - largest - least * (count - 1)
    while spare > 0:
        free = [i for i in range(1, count) if holding[i] < largest] or [i for i in range(1, count) if holding[i] < bound]
        whole, budget = sum([portions[i] for i in free]), spare
        for i in free:
            extra = min(bound - holding[i], max(1, budget * portions[i] // whole), spare)
            holding[i] = holding[i] + extra
            spare = spare - extra
    return np.array(holding)


def bell_draw(rng, shape, width, reach, split=(), kind=jnp.bfloat16):
    entries = jax.random.normal(rng, shape, jnp.float32) * width
    if len(split) > 0:
        entries = levels(rng, shape, split, -0.22, 0.18) * entries
    return jnp.clip(entries, min=-reach, max=reach).astype(kind)


def setup_inputs(seed: int = 0) -> dict:
    streams_of = jax.random.split(jax.random.key(seed), 14)
    queries = draw_queries(jax.random.fold_in(streams_of[13], 71), 0)
    keys = draw_keys(jax.random.fold_in(streams_of[13], 71), 0)
    values = bell_draw(streams_of[2], (SEQUENCE_TOKENS, KEY_VALUE_HEADS * HEAD_SIZE), 1.0, 6.0, ((0, 64), (1, 4)))
    query_gain = draw_query_gain(jax.random.fold_in(streams_of[13], 71), 0)
    key_norm_gain = draw_key_norm_gain(jax.random.fold_in(streams_of[13], 71), 0)
    out_weight = bell_draw(streams_of[5], (QUERY_HEAD_COUNT * HEAD_SIZE, D), (QUERY_HEAD_COUNT * HEAD_SIZE // 4) ** -0.5, 0.25, ((0, 4),))
    residual = bell_draw(streams_of[6], (SEQUENCE_TOKENS, D), 1.0, 6.0, ((0, 256),))
    norm_gain = jnp.clip(1.0 + 0.18 * jax.random.normal(streams_of[7], (D,), jnp.float32), 0.1, 1.9)
    expert_gate = bell_draw(streams_of[8], (EXPERTS, D, FE), D ** -0.5, 0.125, ((0, 64), (2, 4)))
    expert_up = bell_draw(streams_of[9], (EXPERTS, D, FE), D ** -0.5, 0.125, ((0, 64), (2, 4)))
    expert_down = bell_draw(streams_of[10], (EXPERTS, FE, D), FE ** -0.5, 0.109375, ((0, 64), (1, 4)))
    routes_keys = jax.random.split(jax.random.fold_in(streams_of[11], 1), SEQUENCE_TOKENS // (TOK_DEV // N_TP))
    routes_turns = jax.random.permutation(jax.random.fold_in(streams_of[11], 3), SEQUENCE_TOKENS // (TOK_DEV // N_TP))
    routes = jax.vmap(lambda own, number: assign_block(jax.random.fold_in(streams_of[11], 2), own, number, TOK_DEV // N_TP, EXPERTS, TOP, CAP, 2))(routes_keys, routes_turns).reshape((SEQUENCE_TOKENS, TOP))
    route_weight = jnp.clip(0.25 + 0.75 * jax.random.uniform(streams_of[12], (SEQUENCE_TOKENS, TOP), jnp.float32) ** levels(streams_of[12], (SEQUENCE_TOKENS, TOP), ((0, 256),), -0.2, 0.2), 0.25, 1.0)
    return {"queries": queries, "keys": keys, "values": values, "query_gain": query_gain, "key_norm_gain": key_norm_gain, "out_weight": out_weight, "residual": residual, "norm_gain": norm_gain, "expert_gate": expert_gate, "expert_up": expert_up, "expert_down": expert_down, "routes": routes, "route_weight": route_weight}


norm_eps = 1e-06
theta_base = 10000.0

def round_to_half(array):
    return lax.optimization_barrier(array.astype(jnp.bfloat16)).astype(jnp.float32)

def head_normalize(packed, gain, heads):
    heads_float = packed.astype(jnp.float32).reshape(packed.shape[0], heads, HEAD_SIZE)
    scaled = heads_float * lax.rsqrt(lax.optimization_barrier(jnp.mean(heads_float * heads_float, axis=-1, keepdims=True)) + norm_eps)
    return scaled * gain.astype(jnp.float32)

def rotary_tables(positions):
    freq_count = HEAD_SIZE // 4
    grid_row = (positions // GRID_W).astype(jnp.float32)
    grid_col = (positions % GRID_W).astype(jnp.float32)
    inverse = theta_base ** (-jnp.arange(freq_count, dtype=jnp.float32) * 2.0 / (HEAD_SIZE // 2))
    by_row = grid_row[:, None] * inverse
    by_col = grid_col[:, None] * inverse
    angles = jnp.concatenate([by_row, by_row, by_col, by_col], axis=-1)
    return (jnp.cos(angles), jnp.sin(angles))

def apply_rotation(heads_float, cosine_table, sine_values):
    freq_count = HEAD_SIZE // 4
    split_head = heads_float.reshape(heads_float.shape[:-1] + (2, 2, freq_count))
    turned = jnp.stack([-split_head[..., 1, :], split_head[..., 0, :]], axis=-2).reshape(heads_float.shape)
    return heads_float * cosine_table[:, None, :] + turned * sine_values[:, None, :]

def reference(queries, keys, values, query_gain, key_norm_gain, out_weight, residual, norm_gain, expert_gate, expert_up, expert_down, routes, route_weight):
    score_scale = 1.0 / math.sqrt(HEAD_SIZE)
    group_members = QUERY_HEAD_COUNT // KEY_VALUE_HEADS
    positions = jnp.arange(SEQUENCE_TOKENS, dtype=jnp.int32)
    cosine_table, sine_values = rotary_tables(positions)
    rotated_queries = apply_rotation(head_normalize(queries, query_gain, QUERY_HEAD_COUNT), cosine_table, sine_values).astype(jnp.bfloat16)
    rotated_keys = round_to_half(apply_rotation(head_normalize(keys, key_norm_gain, KEY_VALUE_HEADS), cosine_table, sine_values))
    value_wide_float = values.reshape(SEQUENCE_TOKENS, KEY_VALUE_HEADS, HEAD_SIZE).astype(jnp.float32)
    query_tile_rows = math.gcd(SEQUENCE_TOKENS, 128)
    block_list = rotated_queries.reshape(SEQUENCE_TOKENS // query_tile_rows, query_tile_rows, KEY_VALUE_HEADS, group_members, HEAD_SIZE)

    def attend(query_part):
        scores = jnp.einsum('qkgd,skd->kgqs', query_part.astype(jnp.float32), rotated_keys) * score_scale
        row_max = lax.optimization_barrier(jnp.max(scores, axis=-1, keepdims=True))
        weights = jnp.exp(scores - row_max)
        norm_sum = lax.optimization_barrier(jnp.sum(weights, axis=-1))
        value_sum = jnp.einsum('kgqs,skd->kgqd', round_to_half(weights), value_wide_float)
        result = value_sum / norm_sum[..., None]
        return result.transpose(2, 0, 1, 3).reshape(query_tile_rows, QUERY_HEAD_COUNT * HEAD_SIZE).astype(jnp.bfloat16)
    attention = lax.map(attend, block_list).reshape(SEQUENCE_TOKENS, QUERY_HEAD_COUNT * HEAD_SIZE)
    projected = jnp.dot(attention, out_weight, preferred_element_type=jnp.float32)
    hidden_state = residual.astype(jnp.float32) + projected
    normed = (hidden_state * lax.rsqrt(lax.optimization_barrier(jnp.mean(hidden_state * hidden_state, axis=-1, keepdims=True)) + norm_eps) * norm_gain.astype(jnp.float32)).astype(jnp.bfloat16)
    slots_most = N_SP * N_TP * CAP
    flat_routes = routes.reshape(-1)
    flat_weight = route_weight.reshape(-1).astype(jnp.float32)
    piece_width = FE // N_TP

    def expert_step(total, inputs):
        expert, gate_weight, up_weight, down_weight = inputs
        chosen = flat_routes == expert
        route_index = jnp.nonzero(chosen, size=slots_most, fill_value=0)[0].astype(jnp.int32)
        live_mask = (jnp.arange(slots_most, dtype=jnp.int32) < jnp.sum(chosen.astype(jnp.int32))).astype(jnp.float32)
        owner_row = route_index // TOP
        rows_in = normed[owner_row]
        gate_proj = jnp.dot(rows_in, gate_weight, preferred_element_type=jnp.float32)
        up_proj = jnp.dot(rows_in, up_weight, preferred_element_type=jnp.float32)
        hidden_act = (jax.nn.silu(gate_proj) * up_proj).astype(jnp.bfloat16)
        summed = jnp.zeros((slots_most, D), jnp.float32)
        for quarter in range(N_TP):
            down_part = jnp.dot(hidden_act[:, quarter * piece_width:(quarter + 1) * piece_width], down_weight[quarter * piece_width:(quarter + 1) * piece_width], preferred_element_type=jnp.float32)
            summed = summed + round_to_half(down_part)
        output = round_to_half(summed)
        total = total.at[owner_row].add((flat_weight[route_index] * live_mask)[:, None] * output)
        return (total, None)
    moe_sum, _ = lax.scan(expert_step, jnp.zeros((SEQUENCE_TOKENS, D), jnp.float32), (jnp.arange(EXPERTS, dtype=jnp.int32), expert_gate, expert_up, expert_down))
    return (hidden_state + moe_sum).astype(jnp.bfloat16)
```

```python
import functools
import math

import jax
import jax.numpy as jnp
import numpy as np
from jax import lax
from jax.experimental import pallas as pl
from jax.experimental.pallas import tpu as pltpu
from jax.sharding import PartitionSpec as P

HEAD_SIZE = 128
GRID_W = 64
NZ, NY = 8, 4
MESH = pl.DeviceIdType.MESH

norm_eps = 1e-06
theta_base = 10000.0


def _signed(count):
    half = count // 2
    return [0] + [s * m for m in range(1, half) for s in (1, -1)] + [half]


ORDER = sorted(
    [(dz, dy) for dz in _signed(NZ) for dy in _signed(NY)],
    key=lambda d: (abs(d[0]) + abs(d[1]), min(abs(d[0]), abs(d[1]))),
)


def _onward(d, count):
    half = count // 2
    if d == 0:
        return [(1, 0), (1, 1), (-1, 0), (-1, 1)]
    if d == half:
        return []
    if d > 0:
        return [(1, 0)] if d == half - 1 else [(1, 0), (1, 1)]
    return [(-1, 1)] if d == 1 - half else [(-1, 0), (-1, 1)]


def forwards(core, dz, dy):
    both = [(1, 0), (1, 1), (-1, 0), (-1, 1)]
    out = []
    if core == 0:
        if dy == 0:
            out += [("z", s, p) for s, p in _onward(dz, NZ)]
            out += [("y", s, p) for s, p in both]
        else:
            out += [("y", s, p) for s, p in _onward(dy, NY)]
    else:
        if dz == 0:
            out += [("y", s, p) for s, p in _onward(dy, NY)]
            out += [("z", s, p) for s, p in both]
        else:
            out += [("z", s, p) for s, p in _onward(dz, NZ)]
    return out


def attend_kernel(
    q_in, k_in, v_in, qg, kg, rowtab, colcos, colsin, outw_hbm, resid, ng,
    state_out, normed_out,
    kv, q_scr, m_scr, l_scr, acc, outw, part_out, part_in,
    send_sem, recv_sem, w_sem, xs_sem, xr_sem,
):
    me = lax.axis_index("sp")
    t = lax.axis_index("tp")
    z, y, c = me // 8, (me // 2) % NY, me % 2
    chip = me // 2

    wcopy = pltpu.make_async_copy(outw_hbm, outw, w_sem)
    wcopy.start()

    def sp_of(zz, yy, cc):
        return (zz % NZ) * 8 + (yy % NY) * 2 + cc

    near = {
        ("z", 1): sp_of(z + 1, y, c),
        ("z", -1): sp_of(z + NZ - 1, y, c),
        ("y", 1): sp_of(z, y + 1, c),
        ("y", -1): sp_of(z, y + NY - 1, c),
    }
    mate = sp_of(z, y, 1 - c)

    barrier = pltpu.get_barrier_semaphore()
    for peer in list(near.values()) + [mate]:
        pl.semaphore_signal(barrier, inc=1, device_id=(peer, t), device_id_type=MESH)
    for k in range(1, 4):
        pl.semaphore_signal(barrier, inc=1, device_id=(me, (t + k) % 4), device_id_type=MESH)

    lane = lax.broadcasted_iota(jnp.int32, (64, 128), 1)
    low = lane < 64

    def table(row, col):
        return jnp.concatenate(
            [
                jnp.where(low, jnp.broadcast_to(rowtab[row : row + 1, :], (64, 128)), col),
                jnp.where(low, jnp.broadcast_to(rowtab[row + 1 : row + 2, :], (64, 128)), col),
            ],
            axis=0,
        )

    cos = table(0, colcos[...])
    sin = table(2, colsin[...])
    even = ((lax.broadcasted_iota(jnp.int32, (128, 128), 1) // 32) % 2) == 0
    sin_a = jnp.where(even, -sin, 0.0)
    sin_b = jnp.where(even, 0.0, sin)

    def turn(x, gain):
        x = x.astype(jnp.float32)
        x = x * lax.rsqrt(jnp.mean(x * x, axis=-1, keepdims=True) + norm_eps) * gain
        return x * cos + pltpu.roll(x, 96, 1) * sin_a + pltpu.roll(x, 32, 1) * sin_b

    key = turn(k_in[...], kg[...]).astype(jnp.bfloat16).astype(jnp.float32)
    kv[chip, c, 0] = jnp.transpose(key).astype(jnp.bfloat16)
    kv[chip, c, 1] = v_in[...]
    pl.semaphore_wait(barrier, 8)

    def remote(slot, core, part, peer, group):
        return pltpu.make_async_remote_copy(
            src_ref=kv.at[slot, core, part],
            dst_ref=kv.at[slot, core, part],
            send_sem=send_sem.at[group],
            recv_sem=recv_sem.at[slot, core, part],
            device_id=(peer, t),
            device_id_type=MESH,
        )

    def slot_at(dz, dy):
        return ((z + NZ - dz) % NZ) * NY + (y + NY - dy) % NY

    def take(dz, dy):
        slot = slot_at(dz, dy)
        for part in range(2):
            if (dz, dy) != (0, 0):
                remote(slot, c, part, mate, 2).wait_recv()
        for core in range(2):
            @pl.when(c == core)
            def _():
                for axis, sign, part in forwards(core, dz, dy):
                    remote(slot, core, part, near[axis, sign], part).start()
        for part in range(2):
            remote(slot, c, part, mate, 2).start()

    take(*ORDER[0])

    for h in range(4):
        q_scr[h * 128 : (h + 1) * 128, :] = turn(
            q_in[:, h * 128 : (h + 1) * 128], qg[...]
        ).astype(jnp.bfloat16)
    m_scr[...] = jnp.full((512, 128), -1e30, jnp.float32)
    l_scr[...] = jnp.zeros((512, 128), jnp.float32)
    acc[...] = jnp.zeros((512, 128), jnp.float32)
    scale = math.log2(math.e) / math.sqrt(HEAD_SIZE)

    def step(i, carry):
        for k in range(1, 32):
            @pl.when(i == k - 1)
            def _():
                take(*ORDER[k])
        slot = slot_at(*ORDER[0])
        for k in range(1, 32):
            slot = jnp.where(i == k, slot_at(*ORDER[k]), slot)
        for part in range(2):
            remote(slot, 1 - c, part, mate, 2).wait_recv()
        kt = jnp.concatenate([kv[slot, 0, 0], kv[slot, 1, 0]], axis=1)
        vv = jnp.concatenate([kv[slot, 0, 1], kv[slot, 1, 1]], axis=0)
        s = jnp.dot(q_scr[...], kt, preferred_element_type=jnp.float32)
        before = m_scr[...]
        now = jnp.maximum(before, jnp.max(s, axis=1, keepdims=True))
        m_scr[...] = now
        shrink = jnp.exp2((before - now) * scale)
        p = jnp.exp2((s - jnp.concatenate([now, now], axis=1)) * scale)
        l_scr[...] = l_scr[...] * shrink + (p[:, :128] + p[:, 128:])
        acc[...] = acc[...] * shrink + jnp.dot(
            p.astype(jnp.bfloat16), vv, preferred_element_type=jnp.float32
        )
        return carry

    lax.fori_loop(0, 32, step, 0)

    total = jnp.sum(l_scr[...], axis=1, keepdims=True)
    att = (acc[...] / total).astype(jnp.bfloat16)
    att = jnp.concatenate([att[h * 128 : (h + 1) * 128, :] for h in range(4)], axis=1)
    wcopy.wait()
    proj = jnp.dot(att, outw[...], preferred_element_type=jnp.float32).astype(jnp.bfloat16)
    part_out[...] = proj.reshape(4, 32, 2048)

    def cross(k):
        to = (t + k) % 4
        return pltpu.make_async_remote_copy(
            src_ref=part_out.at[to],
            dst_ref=part_in.at[k - 1],
            send_sem=xs_sem.at[k - 1],
            recv_sem=xr_sem.at[k - 1],
            device_id=(me, to),
            device_id_type=MESH,
        )

    for k in (2, 1, 3):
        cross(k).start()
    state = resid[...].astype(jnp.float32) + part_out[t].astype(jnp.float32)
    for k in (1, 3, 2):
        cross(k).wait_recv()
        state = state + part_in[k - 1].astype(jnp.float32)
    state_out[...] = state
    normed_out[...] = (
        state * lax.rsqrt(jnp.mean(state * state, axis=-1, keepdims=True) + norm_eps) * ng[...]
    ).astype(jnp.bfloat16)
    for k in range(1, 4):
        cross(k).wait_send()
    for part in range(2):
        sent = kv.at[0:31, 0, part]
        pltpu.make_async_copy(sent, sent, send_sem.at[part]).wait()
    pltpu.make_async_copy(kv.at[0:16], kv.at[0:16], send_sem.at[2]).wait()


def attend(queries, keys, values, query_gain, key_norm_gain, out_weight, residual, norm_gain):
    inverse = (theta_base ** (-np.arange(32, dtype=np.float64) * 2.0 / 64)).astype(np.float32)
    row = 2 * lax.axis_index("sp") + jnp.arange(2, dtype=jnp.int32)
    by_row = jnp.tile(row.astype(jnp.float32)[:, None] * inverse, (1, 4))
    rowtab = jnp.concatenate([jnp.cos(by_row), jnp.sin(by_row)], axis=0)
    by_col = np.tile(np.arange(64, dtype=np.float32)[:, None] * inverse, (1, 4))
    colcos = jnp.asarray(np.cos(by_col.astype(np.float64)).astype(np.float32))
    colsin = jnp.asarray(np.sin(by_col.astype(np.float64)).astype(np.float32))
    vm = pl.BlockSpec(memory_space=pltpu.VMEM)
    return pl.pallas_call(
        attend_kernel,
        out_shape=(
            jax.ShapeDtypeStruct((32, 2048), jnp.float32),
            jax.ShapeDtypeStruct((32, 2048), jnp.bfloat16),
        ),
        in_specs=[vm] * 8 + [pl.BlockSpec(memory_space=pl.ANY)] + [vm] * 2,
        out_specs=(vm, vm),
        scratch_shapes=[
            pltpu.VMEM((32, 2, 2, 128, 128), jnp.bfloat16),
            pltpu.VMEM((512, 128), jnp.bfloat16),
            pltpu.VMEM((512, 128), jnp.float32),
            pltpu.VMEM((512, 128), jnp.float32),
            pltpu.VMEM((512, 128), jnp.float32),
            pltpu.VMEM((512, 2048), jnp.bfloat16),
            pltpu.VMEM((4, 32, 2048), jnp.bfloat16),
            pltpu.VMEM((3, 32, 2048), jnp.bfloat16),
            pltpu.SemaphoreType.DMA((3,)),
            pltpu.SemaphoreType.DMA((32, 2, 2)),
            pltpu.SemaphoreType.DMA,
            pltpu.SemaphoreType.DMA((3,)),
            pltpu.SemaphoreType.DMA((3,)),
        ],
        compiler_params=pltpu.CompilerParams(
            collective_id=0, has_side_effects=True, vmem_limit_bytes=40 * 1024 * 1024
        ),
        name="attend",
    )(
        queries, keys, values, query_gain.reshape(1, -1), key_norm_gain.reshape(1, -1),
        rowtab, colcos, colsin, out_weight, residual, norm_gain.reshape(1, -1),
    )


def sent_collect(value, axis, dim):
    size = lax.axis_size(axis)
    pieces = lax.all_to_all(
        jnp.broadcast_to(value[None], (size, *value.shape)), axis, 0, 0, tiled=True
    )
    dims = list(pieces.shape[1:])
    dims[dim] *= pieces.shape[0]
    return jnp.moveaxis(pieces, 0, dim).reshape(dims)


def on_device(
    queries,
    keys,
    values,
    query_gain,
    key_norm_gain,
    out_weight,
    residual,
    norm_gain,
    expert_gate,
    expert_up,
    expert_down,
    routes,
    route_weight,
):
    local_rows = queries.shape[0]
    out_rows, model_width = residual.shape
    hidden_state, normed = attend(
        queries, keys, values, query_gain, key_norm_gain, out_weight, residual, norm_gain
    )
    route_top = routes.shape[1]
    group_width = lax.axis_size("tp")
    expert_count = lax.axis_size("sp") * expert_gate.shape[0]
    capacity = 2 * max(1, route_top * local_rows // (group_width * expert_count))
    flat_routes = routes.reshape(-1)
    onehot = (flat_routes[:, None] == jnp.arange(expert_count, dtype=jnp.int32)[None, :]).astype(
        jnp.int32
    )
    earlier = jnp.cumsum(onehot, axis=0) - onehot
    slot_rank = jnp.sum(earlier * onehot, axis=1)
    slot_index = flat_routes * capacity + slot_rank
    placer = (
        jnp.arange(expert_count * capacity, dtype=jnp.int32)[:, None] == slot_index[None, :]
    ).astype(jnp.bfloat16)
    route_rows = jnp.repeat(normed, route_top, axis=0)
    buffer = jnp.dot(placer, route_rows, preferred_element_type=jnp.float32).astype(jnp.bfloat16)
    buffer = buffer.reshape(expert_count, capacity, model_width)
    mail_rows = lax.all_to_all(buffer, "sp", split_axis=0, concat_axis=0, tiled=True)
    inbox_rows = sent_collect(mail_rows, "tp", 1)
    source_count = inbox_rows.shape[0]
    rows_in = inbox_rows.reshape(-1, model_width)
    gate_proj = jnp.dot(rows_in, expert_gate[0], preferred_element_type=jnp.float32)
    up_proj = jnp.dot(rows_in, expert_up[0], preferred_element_type=jnp.float32)
    hidden_act = (jax.nn.silu(gate_proj) * up_proj).astype(jnp.bfloat16)
    down_part = jnp.dot(hidden_act, expert_down[0], preferred_element_type=jnp.float32)
    down_part = down_part.reshape(source_count, group_width * capacity, model_width)
    summed = lax.psum_scatter(down_part.astype(jnp.bfloat16), "tp", scatter_dimension=1, tiled=True)
    returned = lax.all_to_all(summed, "sp", split_axis=0, concat_axis=0, tiled=True)
    per_route = jnp.dot(
        placer.T, returned.reshape(-1, model_width), preferred_element_type=jnp.float32
    )
    per_route = per_route.reshape(out_rows, route_top, model_width)
    moe_sum = jnp.sum(route_weight[:, :, None] * per_route, axis=1)
    return (hidden_state + moe_sum).astype(jnp.bfloat16)


def solution(mesh):
    placed = (
        P("sp", "tp"),
        P("sp", "tp"),
        P("sp", "tp"),
        P(),
        P(),
        P("tp", None),
        P(("sp", "tp"), None),
        P(),
        P("sp", None, "tp"),
        P("sp", None, "tp"),
        P("sp", "tp", None),
        P(("sp", "tp"), None),
        P(("sp", "tp"), None),
    )
    return jax.shard_map(
        on_device, mesh=mesh, in_specs=placed, out_specs=P(("sp", "tp"), None), check_vma=False
    )
```

```python
import functools
import math

import jax
import jax.numpy as jnp
import numpy as np
from jax import lax
from jax.experimental import pallas as pl
from jax.experimental.pallas import tpu as pltpu
from jax.sharding import PartitionSpec as P

HEAD_SIZE = 128
GRID_W = 64
NZ, NY = 8, 4
MESH = pl.DeviceIdType.MESH

norm_eps = 1e-06
theta_base = 10000.0


def _signed(count):
    half = count // 2
    return [0] + [s * m for m in range(1, half) for s in (1, -1)] + [half]


ORDER = sorted(
    [(dz, dy) for dz in _signed(NZ) for dy in _signed(NY)],
    key=lambda d: (abs(d[0]) + abs(d[1]), min(abs(d[0]), abs(d[1]))),
)


def _onward(d, count):
    half = count // 2
    if d == 0:
        return [(1, 0), (1, 1), (-1, 0), (-1, 1)]
    if d == half:
        return []
    if d > 0:
        return [(1, 0)] if d == half - 1 else [(1, 0), (1, 1)]
    return [(-1, 1)] if d == 1 - half else [(-1, 0), (-1, 1)]


def forwards(core, dz, dy):
    both = [(1, 0), (1, 1), (-1, 0), (-1, 1)]
    out = []
    if core == 0:
        if dy == 0:
            out += [("z", s, p) for s, p in _onward(dz, NZ)]
            out += [("y", s, p) for s, p in both]
        else:
            out += [("y", s, p) for s, p in _onward(dy, NY)]
    else:
        if dz == 0:
            out += [("y", s, p) for s, p in _onward(dy, NY)]
            out += [("z", s, p) for s, p in both]
        else:
            out += [("z", s, p) for s, p in _onward(dz, NZ)]
    return out


def attend_kernel(
    q_hbm, k_hbm, v_hbm, qg_hbm, kg_hbm, rowtab_hbm, colcos_hbm, colsin_hbm, outw_hbm, resid_hbm, ng_hbm,
    state_out, normed_out,
    q_in, k_in, v_in, qg, kg, rowtab, colcos, colsin, resid, ng,
    kv, q_scr, m_scr, l_scr, acc, outw, part_out, part_in,
    in_sem, send_sem, recv_sem, w_sem, xs_sem, xr_sem,
):
    me = lax.axis_index("sp")
    t = lax.axis_index("tp")
    z, y, c = me // 8, (me // 2) % NY, me % 2
    chip = me // 2

    fetch = [
        pltpu.make_async_copy(s, d, in_sem.at[i])
        for i, (s, d) in enumerate(
            [
                (k_hbm, k_in), (kg_hbm, kg), (rowtab_hbm, rowtab), (colcos_hbm, colcos),
                (colsin_hbm, colsin), (v_hbm, v_in), (q_hbm, q_in), (qg_hbm, qg),
                (resid_hbm, resid), (ng_hbm, ng),
            ]
        )
    ]
    for cp in fetch:
        cp.start()
    wcopy = pltpu.make_async_copy(outw_hbm, outw, w_sem)
    wcopy.start()

    def sp_of(zz, yy, cc):
        return (zz % NZ) * 8 + (yy % NY) * 2 + cc

    near = {
        ("z", 1): sp_of(z + 1, y, c),
        ("z", -1): sp_of(z + NZ - 1, y, c),
        ("y", 1): sp_of(z, y + 1, c),
        ("y", -1): sp_of(z, y + NY - 1, c),
    }
    mate = sp_of(z, y, 1 - c)

    barrier = pltpu.get_barrier_semaphore()
    for peer in list(near.values()) + [mate]:
        pl.semaphore_signal(barrier, inc=1, device_id=(peer, t), device_id_type=MESH)
    for k in range(1, 4):
        pl.semaphore_signal(barrier, inc=1, device_id=(me, (t + k) % 4), device_id_type=MESH)

    for cp in fetch[:6]:
        cp.wait()
    lane = lax.broadcasted_iota(jnp.int32, (64, 128), 1)
    low = lane < 64

    def table(row, col):
        return jnp.concatenate(
            [
                jnp.where(low, jnp.broadcast_to(rowtab[row : row + 1, :], (64, 128)), col),
                jnp.where(low, jnp.broadcast_to(rowtab[row + 1 : row + 2, :], (64, 128)), col),
            ],
            axis=0,
        )

    cos = table(0, colcos[...])
    sin = table(2, colsin[...])
    even = ((lax.broadcasted_iota(jnp.int32, (128, 128), 1) // 32) % 2) == 0
    sin_a = jnp.where(even, -sin, 0.0)
    sin_b = jnp.where(even, 0.0, sin)

    def turn(x, gain):
        x = x.astype(jnp.float32)
        x = x * lax.rsqrt(jnp.mean(x * x, axis=-1, keepdims=True) + norm_eps) * gain
        return x * cos + pltpu.roll(x, 96, 1) * sin_a + pltpu.roll(x, 32, 1) * sin_b

    key = turn(k_in[...], kg[...]).astype(jnp.bfloat16).astype(jnp.float32)
    kv[chip, c, 0] = jnp.transpose(key).astype(jnp.bfloat16)
    kv[chip, c, 1] = v_in[...]
    pl.semaphore_wait(barrier, 8)

    def remote(slot, core, part, peer, group):
        return pltpu.make_async_remote_copy(
            src_ref=kv.at[slot, core, part],
            dst_ref=kv.at[slot, core, part],
            send_sem=send_sem.at[group],
            recv_sem=recv_sem.at[slot, core, part],
            device_id=(peer, t),
            device_id_type=MESH,
        )

    def slot_at(dz, dy):
        return ((z + NZ - dz) % NZ) * NY + (y + NY - dy) % NY

    def take(dz, dy):
        slot = slot_at(dz, dy)
        for part in range(2):
            if (dz, dy) != (0, 0):
                remote(slot, c, part, mate, 2).wait_recv()
        for core in range(2):
            @pl.when(c == core)
            def _():
                for axis, sign, part in forwards(core, dz, dy):
                    remote(slot, core, part, near[axis, sign], part).start()
        for part in range(2):
            remote(slot, c, part, mate, 2).start()

    take(*ORDER[0])
    for cp in fetch[6:]:
        cp.wait()

    for h in range(4):
        q_scr[h * 128 : (h + 1) * 128, :] = turn(
            q_in[:, h * 128 : (h + 1) * 128], qg[...]
        ).astype(jnp.bfloat16)
    m_scr[...] = jnp.full((512, 128), -1e30, jnp.float32)
    l_scr[...] = jnp.zeros((512, 128), jnp.float32)
    acc[...] = jnp.zeros((512, 128), jnp.float32)
    scale = math.log2(math.e) / math.sqrt(HEAD_SIZE)

    def step(i, carry):
        for k in range(1, 32):
            @pl.when(i == k - 1)
            def _():
                take(*ORDER[k])
        slot = slot_at(*ORDER[0])
        for k in range(1, 32):
            slot = jnp.where(i == k, slot_at(*ORDER[k]), slot)
        for part in range(2):
            remote(slot, 1 - c, part, mate, 2).wait_recv()
        kt = jnp.concatenate([kv[slot, 0, 0], kv[slot, 1, 0]], axis=1)
        vv = jnp.concatenate([kv[slot, 0, 1], kv[slot, 1, 1]], axis=0)
        s = jnp.dot(q_scr[...], kt, preferred_element_type=jnp.float32)
        before = m_scr[...]
        now = jnp.maximum(before, jnp.max(s, axis=1, keepdims=True))
        m_scr[...] = now
        shrink = jnp.exp2((before - now) * scale)
        p = jnp.exp2((s - jnp.concatenate([now, now], axis=1)) * scale)
        l_scr[...] = l_scr[...] * shrink + (p[:, :128] + p[:, 128:])
        acc[...] = acc[...] * shrink + jnp.dot(
            p.astype(jnp.bfloat16), vv, preferred_element_type=jnp.float32
        )
        return carry

    lax.fori_loop(0, 32, step, 0)

    total = jnp.sum(l_scr[...], axis=1, keepdims=True)
    att = (acc[...] / total).astype(jnp.bfloat16)
    att = jnp.concatenate([att[h * 128 : (h + 1) * 128, :] for h in range(4)], axis=1)
    wcopy.wait()
    proj = jnp.dot(att, outw[...], preferred_element_type=jnp.float32).astype(jnp.bfloat16)
    part_out[...] = proj.reshape(4, 32, 2048)

    def cross(k):
        to = (t + k) % 4
        return pltpu.make_async_remote_copy(
            src_ref=part_out.at[to],
            dst_ref=part_in.at[k - 1],
            send_sem=xs_sem.at[k - 1],
            recv_sem=xr_sem.at[k - 1],
            device_id=(me, to),
            device_id_type=MESH,
        )

    for k in (2, 1, 3):
        cross(k).start()
    state = resid[...].astype(jnp.float32) + part_out[t].astype(jnp.float32)
    for k in (1, 3, 2):
        cross(k).wait_recv()
        state = state + part_in[k - 1].astype(jnp.float32)
    state_out[...] = state
    normed_out[...] = (
        state * lax.rsqrt(jnp.mean(state * state, axis=-1, keepdims=True) + norm_eps) * ng[...]
    ).astype(jnp.bfloat16)
    for k in range(1, 4):
        cross(k).wait_send()
    for part in range(2):
        sent = kv.at[0:31, 0, part]
        pltpu.make_async_copy(sent, sent, send_sem.at[part]).wait()
    pltpu.make_async_copy(kv.at[0:16], kv.at[0:16], send_sem.at[2]).wait()


def attend(queries, keys, values, query_gain, key_norm_gain, out_weight, residual, norm_gain):
    inverse = (theta_base ** (-np.arange(32, dtype=np.float64) * 2.0 / 64)).astype(np.float32)
    row = 2 * lax.axis_index("sp") + jnp.arange(2, dtype=jnp.int32)
    by_row = jnp.tile(row.astype(jnp.float32)[:, None] * inverse, (1, 4))
    rowtab = jnp.concatenate([jnp.cos(by_row), jnp.sin(by_row)], axis=0)
    by_col = np.tile(np.arange(64, dtype=np.float32)[:, None] * inverse, (1, 4))
    colcos = jnp.asarray(np.cos(by_col.astype(np.float64)).astype(np.float32))
    colsin = jnp.asarray(np.sin(by_col.astype(np.float64)).astype(np.float32))
    vm = pl.BlockSpec(memory_space=pltpu.VMEM)
    return pl.pallas_call(
        attend_kernel,
        out_shape=(
            jax.ShapeDtypeStruct((32, 2048), jnp.float32),
            jax.ShapeDtypeStruct((32, 2048), jnp.bfloat16),
        ),
        in_specs=[pl.BlockSpec(memory_space=pl.ANY)] * 11,
        out_specs=(vm, vm),
        scratch_shapes=[
            pltpu.VMEM((128, 512), jnp.bfloat16),
            pltpu.VMEM((128, 128), jnp.bfloat16),
            pltpu.VMEM((128, 128), jnp.bfloat16),
            pltpu.VMEM((1, 128), jnp.float32),
            pltpu.VMEM((1, 128), jnp.float32),
            pltpu.VMEM((4, 128), jnp.float32),
            pltpu.VMEM((64, 128), jnp.float32),
            pltpu.VMEM((64, 128), jnp.float32),
            pltpu.VMEM((32, 2048), jnp.bfloat16),
            pltpu.VMEM((1, 2048), jnp.float32),
            pltpu.VMEM((32, 2, 2, 128, 128), jnp.bfloat16),
            pltpu.VMEM((512, 128), jnp.bfloat16),
            pltpu.VMEM((512, 128), jnp.float32),
            pltpu.VMEM((512, 128), jnp.float32),
            pltpu.VMEM((512, 128), jnp.float32),
            pltpu.VMEM((512, 2048), jnp.bfloat16),
            pltpu.VMEM((4, 32, 2048), jnp.bfloat16),
            pltpu.VMEM((3, 32, 2048), jnp.bfloat16),
            pltpu.SemaphoreType.DMA((10,)),
            pltpu.SemaphoreType.DMA((3,)),
            pltpu.SemaphoreType.DMA((32, 2, 2)),
            pltpu.SemaphoreType.DMA,
            pltpu.SemaphoreType.DMA((3,)),
            pltpu.SemaphoreType.DMA((3,)),
        ],
        compiler_params=pltpu.CompilerParams(
            collective_id=0, has_side_effects=True, vmem_limit_bytes=40 * 1024 * 1024
        ),
        name="attend",
    )(
        queries, keys, values, query_gain.reshape(1, -1), key_norm_gain.reshape(1, -1),
        rowtab, colcos, colsin, out_weight, residual, norm_gain.reshape(1, -1),
    )


def perm_pair():
    row = lax.broadcasted_iota(jnp.int32, (256, 256), 0)
    col = lax.broadcasted_iota(jnp.int32, (256, 256), 1)
    to_blocks = (((row // 2) % 16) * 16 + (row // 32) * 2 + row % 2) == col
    to_rows = (((col // 2) % 16) * 16 + (col // 32) * 2 + col % 2) == row
    return (
        jnp.where(to_blocks, 1.0, 0.0).astype(jnp.bfloat16),
        jnp.where(to_rows, 1.0, 0.0).astype(jnp.bfloat16),
    )


def moved(perm, value):
    return jnp.dot(perm, value, preferred_element_type=jnp.float32).astype(jnp.bfloat16)


def experts_kernel(
    normed_hbm, state_hbm, rrow_hbm, rcol_hbm, rw_hbm, wg_hbm, wu_hbm, wd_hbm,
    out,
    normed, state, rrow, rcol, rw, wg, wu, wd,
    sb, xb, rows, hid, down, relay_in, relay_out, final_in, ob, cb,
    in_sem, w_sem, a_send, a_recv, x_send, x_recv, r_send, r_recv, b_send, b_recv,
):
    me = lax.axis_index("sp")
    t = lax.axis_index("tp")
    z = me // 8
    right, left = (t + 1) % 4, (t + 3) % 4
    far = (t + 2) % 4

    small = [
        pltpu.make_async_copy(s, d, in_sem.at[i])
        for i, (s, d) in enumerate(
            [(normed_hbm, normed), (rrow_hbm, rrow), (rcol_hbm, rcol), (rw_hbm, rw), (state_hbm, state)]
        )
    ]
    weights = [
        pltpu.make_async_copy(s, d, w_sem.at[i])
        for i, (s, d) in enumerate([(wg_hbm.at[0], wg), (wu_hbm.at[0], wu), (wd_hbm.at[0], wd)])
    ]
    for cp in small + weights:
        cp.start()

    barrier = pltpu.get_barrier_semaphore()

    def hello(k, carry):
        pl.semaphore_signal(
            barrier, inc=1, device_id=((me + k) % 64, t), device_id_type=MESH
        )
        return carry

    lax.fori_loop(1, 64, hello, 0)
    for peer in (right, left):
        pl.semaphore_signal(barrier, inc=1, device_id=(me, peer), device_id_type=MESH)

    to_blocks, to_rows = perm_pair()

    for cp in small:
        cp.wait()
    same = rcol[...] == rrow[...]
    sub = lax.broadcasted_iota(jnp.int32, (64, 64), 0)
    lane = lax.broadcasted_iota(jnp.int32, (64, 64), 1)
    slot_row = rrow[...] * 2 + jnp.sum(
        jnp.where(same & (sub < lane), 1, 0), axis=0, keepdims=True
    )
    slot_col = rcol[...] * 2 + jnp.sum(
        jnp.where(same & (lane < sub), 1, 0), axis=1, keepdims=True
    )
    place = lax.broadcasted_iota(jnp.int32, (128, 32), 0)
    placer = (
        jnp.where(place == slot_row[:, :32], 1.0, 0.0)
        + jnp.where(place == slot_row[:, 32:], 1.0, 0.0)
    ).astype(jnp.bfloat16)
    picker = jnp.where(
        lax.broadcasted_iota(jnp.int32, (64, 128), 1) == slot_col, 1.0, 0.0
    ).astype(jnp.bfloat16)
    mail = moved(placer, normed[...])

    def stacked(value):
        return jnp.concatenate(
            [value[:, ct * 128 : (ct + 1) * 128] for ct in range(16)], axis=0
        )

    for g in range(0, 8, 2):
        pair = jnp.concatenate(
            [stacked(mail[16 * g : 16 * g + 16]), stacked(mail[16 * g + 16 : 16 * g + 32])], axis=1
        )
        pair = moved(to_blocks, pair)
        sb[8 * g : 8 * g + 8] = pair[:, :128].reshape(8, 32, 128)
        sb[8 * g + 8 : 8 * g + 16] = pair[:, 128:].reshape(8, 32, 128)

    def zone(u):
        return (z + 8 + ((u + 1) // 2) * (2 * (u % 2) - 1)) % 8

    xb[t, me] = sb[me]
    pl.semaphore_wait(barrier, 65)

    def post(k, carry):
        u, i = k // 8, k % 8
        to = zone(u) * 8 + (me + i) % 8

        @pl.when(k > 0)
        def _():
            pltpu.make_async_remote_copy(
                src_ref=sb.at[to],
                dst_ref=xb.at[t, me],
                send_sem=a_send,
                recv_sem=a_recv.at[z],
                device_id=(to, t),
                device_id_type=MESH,
            ).start()

        return carry

    lax.fori_loop(0, 64, post, 0)

    def local_wait(ref, sem):
        pltpu.make_async_copy(ref, ref, sem).wait()

    def spread(u, block, lo, n, lane_id, peer):
        src = xb.at[block, pl.ds(zone(u) * 8 + lo, n)]
        return pltpu.make_async_remote_copy(
            src_ref=src,
            dst_ref=src,
            send_sem=x_send.at[u, lane_id],
            recv_sem=x_recv.at[u, lane_id],
            device_id=(me, peer),
            device_id_type=MESH,
        )

    def spread_all(u):
        return (
            spread(u, t, 0, 8, 0, right),
            spread(u, t, 0, 8, 1, left),
            spread(u, left, 0, 4, 2, right),
            spread(u, right, 4, 4, 3, left),
        )

    def arrivals(u):
        return (
            spread(u, left, 0, 8, 0, right),
            spread(u, right, 0, 8, 1, left),
            spread(u, far, 0, 4, 2, right),
            spread(u, far, 4, 4, 3, left),
        )

    def dispatch(i, carry):
        @pl.when(i == 0)
        def _():
            local_wait(xb.at[t, 0:7], a_recv.at[z])

        @pl.when((i > 0) & (i < 8))
        def _():
            local_wait(xb.at[t, 0:8], a_recv.at[zone(i)])

        @pl.when(i < 8)
        def _():
            for cp in spread_all(i)[:2]:
                cp.start()

        @pl.when((i > 0) & (i < 9))
        def _():
            for k in range(2):
                arrivals(i - 1)[k].wait_recv()
                spread_all(i - 1)[2 + k].start()

        @pl.when(i > 1)
        def _():
            u = i - 2
            for k in range(2):
                arrivals(u)[2 + k].wait_recv()
            zi = zone(u)
            at = pl.multiple_of(zi * 16, 16)
            for h in range(0, 4, 2):
                pair = jnp.concatenate(
                    [xb[h + d, pl.ds(zi * 8, 8)].reshape(256, 128) for d in range(2)], axis=1
                )
                pair = moved(to_rows, pair)
                for d in range(2):
                    for ct in range(16):
                        rows[h + d, pl.ds(at, 16), ct * 128 : (ct + 1) * 128] = pair[
                            ct * 16 : ct * 16 + 16, d * 128 : (d + 1) * 128
                        ]

        return carry

    lax.fori_loop(0, 10, dispatch, 0)

    for cp in weights[:2]:
        cp.wait()

    def gate_up(n, carry):
        cols = pl.ds(pl.multiple_of(n * 256, 256), 256)
        x = rows[...].reshape(512, 2048)
        gate = jnp.dot(x, wg[:, cols], preferred_element_type=jnp.float32)
        up = jnp.dot(x, wu[:, cols], preferred_element_type=jnp.float32)
        hid[:, cols] = (gate / (1.0 + jnp.exp(-gate)) * up).astype(jnp.bfloat16)
        return carry

    lax.fori_loop(0, 3, gate_up, 0)
    weights[2].wait()

    def down_tile(n, carry):
        cols = pl.ds(pl.multiple_of(n * 256, 256), 256)
        d = jnp.dot(hid[...], wd[:, cols], preferred_element_type=jnp.float32)
        down[:, :, cols] = d.astype(jnp.bfloat16).reshape(4, 128, 256)
        return carry

    lax.fori_loop(0, 8, down_tile, 0)

    lo, hi = pl.ds(0, 1024), pl.ds(1024, 1024)

    def ring(u, src, dst, lane_id, peer):
        return pltpu.make_async_remote_copy(
            src_ref=src,
            dst_ref=dst,
            send_sem=r_send.at[u, lane_id],
            recv_sem=r_recv.at[u, lane_id],
            device_id=(me, peer),
            device_id_type=MESH,
        )

    def piece(block, u, half):
        return down.at[block, pl.ds(pl.multiple_of(zone(u) * 16, 16), 16), half]

    def first_sends(u):
        return (
            ring(u, piece(far, u, lo), relay_in.at[0, u], 0, right),
            ring(u, piece(far, u, hi), relay_in.at[1, u], 1, left),
            ring(u, piece(right, u, hi), final_in.at[0, u, :, hi], 2, right),
            ring(u, piece(left, u, lo), final_in.at[1, u, :, lo], 3, left),
        )

    def second_sends(u):
        return (
            ring(u, relay_out.at[0, u], final_in.at[0, u, :, lo], 4, right),
            ring(u, relay_out.at[1, u], final_in.at[1, u, :, hi], 5, left),
        )

    def back(u, i):
        to = zone(u) * 8 + (me + i) % 8
        return pltpu.make_async_remote_copy(
            src_ref=ob.at[to],
            dst_ref=cb.at[me],
            send_sem=b_send,
            recv_sem=b_recv,
            device_id=(to, t),
            device_id_type=MESH,
        )

    def combine(i, carry):
        @pl.when(i < 8)
        def _():
            for cp in first_sends(7 - i):
                cp.start()

        @pl.when((i > 0) & (i < 9))
        def _():
            u = 8 - i
            for k, (block, half) in enumerate(((right, lo), (left, hi))):
                first_sends(u)[k].wait_recv()
                at = pl.ds(pl.multiple_of(zone(u) * 16, 16), 16)
                relay_out[k, u] = (
                    relay_in[k, u].astype(jnp.float32) + down[block, at, half].astype(jnp.float32)
                ).astype(jnp.bfloat16)
                second_sends(u)[k].start()

        @pl.when(i > 1)
        def _():
            u = 9 - i
            for cp in first_sends(u)[2:] + second_sends(u):
                cp.wait_recv()
            zi = zone(u)
            at = pl.ds(pl.multiple_of(zi * 16, 16), 16)
            whole = (
                down[t, at, :].astype(jnp.float32)
                + final_in[0, u].astype(jnp.float32)
                + final_in[1, u].astype(jnp.float32)
            ).astype(jnp.bfloat16)
            ob[pl.ds(zi * 8, 8)] = moved(to_blocks, stacked(whole)).reshape(8, 32, 128)

            @pl.when(u == 0)
            def _():
                cb[me] = ob[me]

            for k in range(8):
                if k == 0:
                    @pl.when(u > 0)
                    def _():
                        back(u, 0).start()
                else:
                    back(u, k).start()

        return carry

    lax.fori_loop(0, 10, combine, 0)

    local_wait(cb.at[0:63], b_recv)
    nat = []
    for g in range(0, 8, 2):
        pair = jnp.concatenate(
            [cb[8 * g + 8 * d : 8 * g + 8 * d + 8].reshape(256, 128) for d in range(2)], axis=1
        )
        pair = moved(to_rows, pair)
        for d in range(2):
            nat.append(
                jnp.concatenate(
                    [
                        pair[ct * 16 : ct * 16 + 16, d * 128 : (d + 1) * 128]
                        for ct in range(16)
                    ],
                    axis=1,
                )
            )
    nat = jnp.concatenate(nat, axis=0)
    picked = jnp.dot(picker, nat, preferred_element_type=jnp.float32)
    out[...] = (
        state[...] + rw[:, 0:1] * picked[:32] + rw[:, 1:2] * picked[32:]
    ).astype(jnp.bfloat16)

    local_wait(cb.at[0:63], a_send)
    local_wait(cb.at[0:63], b_send)

    def drain(u, carry):
        for cp in spread_all(u) + first_sends(u) + second_sends(u):
            cp.wait_send()
        return carry

    lax.fori_loop(0, 8, drain, 0)


def experts(normed, state, routes, route_weight, expert_gate, expert_up, expert_down):
    flat = routes.T.reshape(1, 64)
    anywhere = pl.BlockSpec(memory_space=pl.ANY)
    bf16, f32, i32 = jnp.bfloat16, jnp.float32, jnp.int32
    dma = pltpu.SemaphoreType.DMA
    return pl.pallas_call(
        experts_kernel,
        out_shape=jax.ShapeDtypeStruct((32, 2048), bf16),
        in_specs=[anywhere] * 8,
        out_specs=pl.BlockSpec(memory_space=pltpu.VMEM),
        scratch_shapes=[
            pltpu.VMEM((32, 2048), bf16),
            pltpu.VMEM((32, 2048), f32),
            pltpu.VMEM((1, 64), i32),
            pltpu.VMEM((64, 1), i32),
            pltpu.VMEM((32, 2), f32),
            pltpu.VMEM((2048, 768), bf16),
            pltpu.VMEM((2048, 768), bf16),
            pltpu.VMEM((768, 2048), bf16),
            pltpu.VMEM((64, 32, 128), bf16),
            pltpu.VMEM((4, 64, 32, 128), bf16),
            pltpu.VMEM((4, 128, 2048), bf16),
            pltpu.VMEM((512, 768), bf16),
            pltpu.VMEM((4, 128, 2048), bf16),
            pltpu.VMEM((2, 8, 16, 1024), bf16),
            pltpu.VMEM((2, 8, 16, 1024), bf16),
            pltpu.VMEM((2, 8, 16, 2048), bf16),
            pltpu.VMEM((64, 32, 128), bf16),
            pltpu.VMEM((64, 32, 128), bf16),
            dma((5,)),
            dma((3,)),
            dma,
            dma((8,)),
            dma((8, 4)),
            dma((8, 4)),
            dma((8, 6)),
            dma((8, 6)),
            dma,
            dma,
        ],
        compiler_params=pltpu.CompilerParams(
            collective_id=1, has_side_effects=True, vmem_limit_bytes=56 * 1024 * 1024
        ),
        name="experts",
    )(
        normed, state, flat, flat.reshape(64, 1), route_weight,
        expert_gate, expert_up, expert_down,
    )


def on_device(
    queries,
    keys,
    values,
    query_gain,
    key_norm_gain,
    out_weight,
    residual,
    norm_gain,
    expert_gate,
    expert_up,
    expert_down,
    routes,
    route_weight,
):
    state, normed = attend(
        queries, keys, values, query_gain, key_norm_gain, out_weight, residual, norm_gain
    )
    return experts(normed, state, routes, route_weight, expert_gate, expert_up, expert_down)


def solution(mesh):
    placed = (
        P("sp", "tp"),
        P("sp", "tp"),
        P("sp", "tp"),
        P(),
        P(),
        P("tp", None),
        P(("sp", "tp"), None),
        P(),
        P("sp", None, "tp"),
        P("sp", None, "tp"),
        P("sp", "tp", None),
        P(("sp", "tp"), None),
        P(("sp", "tp"), None),
    )
    return jax.shard_map(
        on_device, mesh=mesh, in_specs=placed, out_specs=P(("sp", "tp"), None), check_vma=False
    )
```
